32 devices in a mesh: ep: 8 (over z, y), tp: 4 (over x, core).
Axes of the slice: x: 2, y: 2, z: 4, core: 2. Of those that a mesh axis runs over, the one named last changes fastest.
Arguments:
- tokens: bfloat16 [2048, 2048], P('ep', 'tp'), may hold values from -400 to 400
- expert_ids: int32 [2048, 2], P('ep'), may hold values from 0 to 7, all different within a row; in each aligned block of 256 rows (0 to 255, 256 to 511, ...) at most 80 rows name the same one
- route_weights: float32 [2048, 2], P('ep'), may hold values from 0.1 to 1
- pre_gain: float32 [2048], P('tp'), may hold values from 0.1 to 1.9
- post_gain: float32 [2048], P('tp'), may hold values from 0.1 to 1.9
- gate_weight: bfloat16 [8, 2048, 4096], P('ep', None, 'tp'), may hold values from -0.125 to 0.125
- up_weight: bfloat16 [8, 2048, 4096], P('ep', None, 'tp'), may hold values from -0.125 to 0.125
- down_weight: bfloat16 [8, 4096, 2048], P('ep', None, 'tp'), may hold values from -0.71875 to 0.71875
Outputs:
- layer_out: bfloat16 [2048, 2048], P('ep', 'tp')
The draws below stay inside these ranges and needn't reach their ends.
Inputs may be any that keep to these rules, and one draw needn't show every extreme that they name: `expert_ids`: the 2 experts of a token are distinct. Within the rows of one device along ep, no expert is named more than 80 times, a bound that some block reaches.
All inputs are finite; a program needn't handle non-finite values.
Results may differ from the reference program's by a relative error of at most 0.007.
Values may be sent and summed in bfloat16 or wider, within the bound.
A program may use at most 64 MiB of HBM per device.

```python
import math
import jax
import jax.numpy as jnp
import numpy as np
from jax import lax

D = 2048
DE = 4096
TOPK = 2
TOK_DEV = 256
EXPERTS = 8
TOKENS = 2048
CAP = 80
N_EP = 8


def draw_tokens(key, part):
    first, second, third = jax.random.split(jax.random.fold_in(key, 11), 3)
    base = jnp.clip(jax.random.normal(first, (TOKENS, D), jnp.float32), -6.0, 6.0)
    rising = jnp.exp(jnp.log(4.0) * jnp.arange(D, dtype=jnp.float32) / D)
    rough = jax.random.uniform(second, (1, D), jnp.float32, 0.5, 1.5)
    row_scale = jnp.exp(jax.random.uniform(third, (TOKENS, 1), jnp.float32, 0.0, jnp.log(10.0)))
    return (base * rising[None, :] * rough * row_scale).astype(jnp.bfloat16)


def draw_down_weight(key, part):
    first, second = jax.random.split(jax.random.fold_in(key, 23), 2)
    base = jnp.clip(jax.random.normal(first, (EXPERTS, DE, D), jnp.float32), -6.0, 6.0)
    rising = jnp.exp(jnp.log(5.0) * jnp.arange(D, dtype=jnp.float32) / D)
    rough = jax.random.uniform(second, (1, 1, D), jnp.float32, 0.5, 1.5)
    return (base * rising[None, None, :] * rough * DE ** (-0.5)).astype(jnp.bfloat16)


def steps_of(stream_key, dims, cuts, smallest, top_value):
    level, own = 1.0, jax.random.fold_in(stream_key, 6)
    for axis_at, parts in cuts:
        steps = jnp.exp(jax.random.uniform(jax.random.fold_in(own, axis_at), (parts,), jnp.float32, smallest / len(cuts), top_value / len(cuts)))
        level = level * jnp.repeat(steps, dims[axis_at] // parts).reshape([-1 if axis == axis_at else 1 for axis in range(len(dims))])
    return level


def assign_block(key, own, number, rows, count, top, reach, skew):
    order = jax.random.permutation(key, count)
    packed, common = load_shares(count, rows * top, reach, skew, True), load_shares(count, rows * top, reach, skew, False)
    places = jnp.arange(count)

    def named(tallies, turn):
        used = int((tallies > 0).sum())
        fixed = max(1, used // 4)
        moved = fixed + (places - fixed + turn * (used - fixed)) % max(1, count - fixed)
        return jnp.zeros((count,), jnp.int32).at[order[jnp.where(places < fixed, places, moved)]].set(jnp.asarray(tallies, jnp.int32))

    tallies = jnp.where(number % 4 == 0, named(packed, number // 4), named(common, number - number // 4 - 1))
    mixed = jax.random.permutation(jax.random.fold_in(own, 3), count)
    giver, receiver = mixed[0:count // 2 * 2:2], mixed[1:count // 2 * 2:2]
    margin = jnp.minimum(tallies[giver] - 1, reach - tallies[receiver]) // 2
    margin = jnp.where((giver == order[0]) | (receiver == order[0]) | (tallies[receiver] == 0), 0, jnp.maximum(margin, 0))
    moved = jax.random.randint(jax.random.fold_in(own, 4), (count // 2,), 0, 1 << 20) % (margin + 1)
    tallies = tallies.at[giver].add(-moved).at[receiver].add(moved)
    items = jnp.searchsorted(jnp.cumsum(tallies), jnp.arange(rows * top), side="right").astype(jnp.int32)
    grid = items.reshape(top, rows).T
    grid = grid[jax.random.permutation(jax.random.fold_in(own, 1), rows)]
    turn = jax.random.randint(jax.random.fold_in(own, 2), (rows, 1), 0, top)
    return jnp.take_along_axis(grid, (jnp.arange(top)[None, :] + turn) % top, axis=1)


def load_shares(count, total, bound, skew, full):
    portions = [(1 << 20) // math.isqrt(standing ** skew) + 1 for standing in range(1, count + 1)]
    largest = bound if full else min(bound, max(-(-total // count), total * portions[0] // sum(portions)))
    least = 1 if total - largest >= count - 1 else 0
    given, spare = [largest] + [least] * (count - 1), total - largest - least * (count - 1)
    while spare > 0:
        free = [i for i in range(1, count) if given[i] < largest] or [i for i in range(1, count) if given[i] < bound]
        mass, remaining = sum([portions[i] for i in free]), spare
        for i in free:
            addition = min(bound - given[i], max(1, remaining * portions[i] // mass), spare)
            given[i] = given[i] + addition
            spare = spare - addition
    return np.array(given)


def bell_draw(own_key, extent, width, most, cuts=(), kind=jnp.bfloat16):
    result = width * jax.random.normal(own_key, extent, jnp.float32)
    if cuts:
        result = result * steps_of(own_key, extent, cuts, -0.22, 0.18)
    return jnp.clip(result, -most, most).astype(kind)


def setup_inputs(seed: int = 0) -> dict:
    streams_of = jax.random.split(jax.random.key(seed), 9)
    tokens = draw_tokens(jax.random.fold_in(streams_of[8], 71), 0)
    expert_ids_keys = jax.random.split(jax.random.fold_in(streams_of[1], 1), TOKENS // TOK_DEV)
    expert_ids_turns = jax.random.permutation(jax.random.fold_in(streams_of[1], 3), TOKENS // TOK_DEV)
    expert_ids = jax.vmap(lambda own, number: assign_block(jax.random.fold_in(streams_of[1], 2), own, number, TOK_DEV, EXPERTS, TOPK, CAP, 2))(expert_ids_keys, expert_ids_turns).reshape((TOKENS, TOPK))
    route_weights = jnp.clip(0.1 + 0.9 * jax.random.uniform(streams_of[2], (TOKENS, TOPK), jnp.float32) ** steps_of(streams_of[2], (TOKENS, TOPK), ((0, 8),), -0.2, 0.2), 0.1, 1.0)
    pre_gain = jnp.clip(1.0 + 0.18 * jax.random.normal(streams_of[3], (D,), jnp.float32), 0.1, 1.9)
    post_gain = jnp.clip(1.0 + 0.18 * jax.random.normal(streams_of[4], (D,), jnp.float32), 0.1, 1.9)
    gate_weight = bell_draw(streams_of[5], (EXPERTS, D, DE), D ** -0.5, 0.125, ((0, 8), (2, 4)))
    up_weight = bell_draw(streams_of[6], (EXPERTS, D, DE), D ** -0.5, 0.125, ((0, 8), (2, 4)))
    down_weight = draw_down_weight(jax.random.fold_in(streams_of[8], 71), 0)
    return {"tokens": tokens, "expert_ids": expert_ids, "route_weights": route_weights, "pre_gain": pre_gain, "post_gain": post_gain, "gate_weight": gate_weight, "up_weight": up_weight, "down_weight": down_weight}


epsilon = 1e-06

def reference(tokens, expert_ids, route_weights, pre_gain, post_gain, gate_weight, up_weight, down_weight):
    tok_float = tokens.astype(jnp.float32)
    mean_in = lax.optimization_barrier(jnp.mean(tok_float * tok_float, axis=1, keepdims=True))
    normed = (tok_float * lax.rsqrt(mean_in + epsilon) * pre_gain.astype(jnp.float32)[None, :]).astype(jnp.bfloat16)
    pairs = N_EP * TOK_DEV * TOPK
    blocks = expert_ids.reshape(N_EP, TOK_DEV * TOPK)
    onehot = (blocks[:, :, None] == jnp.arange(EXPERTS, dtype=jnp.int32)[None, None, :]).astype(jnp.int32)
    slot = lax.optimization_barrier(jnp.sum((jnp.cumsum(onehot, axis=1) - 1) * onehot, axis=2)).astype(jnp.int32).reshape(-1)
    block_of = jnp.arange(pairs, dtype=jnp.int32) // (TOK_DEV * TOPK)
    flat_ids = expert_ids.reshape(-1).astype(jnp.int32)
    row_of = (block_of * CAP + slot).astype(jnp.int32)
    token_of = jnp.arange(pairs, dtype=jnp.int32) // TOPK
    table = jnp.full((EXPERTS, N_EP * CAP), TOKENS, jnp.int32).at[flat_ids, row_of].set(token_of)
    padded = jnp.concatenate([normed, jnp.zeros((1, D), jnp.bfloat16)], axis=0)

    def expert(inputs):
        row_index, w_gate, w_up, w_down = inputs
        rows = padded[row_index].astype(jnp.float32)
        gate = jnp.dot(rows, w_gate.astype(jnp.float32))
        upper = jnp.dot(rows, w_up.astype(jnp.float32))
        hidden = (jax.nn.silu(gate) * upper).astype(jnp.bfloat16)
        return jnp.dot(hidden.astype(jnp.float32), w_down.astype(jnp.float32)).astype(jnp.bfloat16)
    results = lax.map(expert, (table, gate_weight, up_weight, down_weight))
    picked = results[flat_ids, row_of].reshape(TOKENS, TOPK, D).astype(jnp.float32)
    mixed = lax.optimization_barrier(jnp.sum(picked * route_weights.astype(jnp.float32)[:, :, None], axis=1))
    mean_out = lax.optimization_barrier(jnp.mean(mixed * mixed, axis=1, keepdims=True))
    return (mixed * lax.rsqrt(mean_out + epsilon) * post_gain.astype(jnp.float32)[None, :]).astype(jnp.bfloat16)
```

```python
import functools

import jax
import jax.numpy as jnp
from jax import lax
from jax.experimental import pallas as pl
from jax.experimental.pallas import tpu as pltpu
from jax.sharding import PartitionSpec as P

epsilon = 1e-06
MESH = pl.DeviceIdType.MESH
f32, bf16 = jnp.float32, jnp.bfloat16


def flip(index, bits):
    out, bit = index, 1
    while bit <= bits:
        if bits & bit:
            out = out + bit * (1 - 2 * ((index // bit) % 2))
        bit *= 2
    return out


def to_column(row):
    return jnp.transpose(jnp.broadcast_to(row, (128, row.shape[1])))


def row_sums(values):
    part = values[:, 0:128]
    for at in range(128, values.shape[1], 128):
        part = part + values[:, at : at + 128]
    return jnp.sum(jnp.transpose(part), axis=0, keepdims=True)


def kernel(
    n, tp, capacity, cap, groups, order,
    tok_ref, ids_ref, rw_ref, pre_ref, post_ref, wg_hbm, wu_hbm, wd_hbm,
    out_ref,
    wg, wu, wd, outg, feats, hid, back, ret, pick, ss_in, ss_out,
    w_sem, si_s, si_r, so_s, so_r, d_s, d_r, fx_s, fx_r, fp_s, fp_r,
    hx_s, hx_r, hp_s, hp_r, r_s, r_r,
):
    me, ti = lax.axis_index("ep"), lax.axis_index("tp")
    chips = tp // 2
    chip, core = ti // 2, ti % 2
    partner = chip * 2 + (1 - core)
    rows, width = tok_ref.shape
    units = wg.shape[1]
    n_tile = min(256, units)
    tiles = units // n_tile
    per_group = n // groups
    group_rows = per_group * cap

    barrier = pltpu.get_barrier_semaphore()
    for d in range(1, n):
        pl.semaphore_signal(barrier, inc=1, device_id={"ep": flip(me, d)}, device_id_type=MESH)
    for j in range(1, tp):
        pl.semaphore_signal(barrier, inc=1, device_id={"tp": (ti + j) % tp}, device_id_type=MESH)
    loads = [
        pltpu.make_async_copy(src.at[0], dst, w_sem.at[i])
        for i, (src, dst) in enumerate(((wg_hbm, wg), (wu_hbm, wu), (wd_hbm, wd)))
    ]
    for load in loads:
        load.start()
    sent = []

    def remote(src, dst, s_sem, r_sem, where):
        return pltpu.make_async_remote_copy(
            src_ref=src, dst_ref=dst, send_sem=s_sem, recv_sem=r_sem,
            device_id=where, device_id_type=MESH,
        )

    def go(copy):
        copy.start()
        sent.append(copy)

    def total_over_tp(buf, s_sem, r_sem, row, before_wait=None):
        buf[0] = row
        if before_wait is not None:
            before_wait()
        copies = [
            remote(buf.at[0], buf.at[j], s_sem.at[j], r_sem.at[j], {"tp": (ti + j) % tp})
            for j in range(1, tp)
        ]
        for copy in copies:
            go(copy)
        return copies

    tok = tok_ref[...].astype(f32)
    square_row = row_sums(tok * tok)
    in_copies = total_over_tp(
        ss_in, si_s, si_r, square_row,
        lambda: pl.semaphore_wait(barrier, n - 1 + tp - 1),
    )

    lanes = max(n, 16)
    rel = [jnp.bitwise_xor(ids_ref[k : k + 1, :], me) for k in range(2)]
    d_iota = lax.broadcasted_iota(jnp.int32, (lanes, rows), 0)
    hot = [jnp.where(rel[k] == d_iota, 1.0, 0.0).astype(f32) for k in range(2)]
    earlier = jnp.where(
        lax.broadcasted_iota(jnp.int32, (rows, rows), 0)
        < lax.broadcasted_iota(jnp.int32, (rows, rows), 1), 1.0, 0.0,
    ).astype(bf16)
    prefix = jnp.dot((hot[0] + hot[1]).astype(bf16), earlier, preferred_element_type=f32)
    target = [
        rel[k].astype(f32) * cap + jnp.sum(prefix * hot[k], axis=0, keepdims=True)
        for k in range(2)
    ]
    slot_iota = lax.broadcasted_iota(jnp.int32, (cap, rows), 0).astype(f32)

    for copy in in_copies:
        copy.wait_recv()
    total = ss_in[0]
    for j in range(1, tp):
        total = total + ss_in[j]
    scale = to_column(lax.rsqrt(total / (width * tp) + epsilon))[:, 0:1]
    normed = (tok_ref[...].astype(f32) * scale * pre_ref[...]).astype(bf16)

    own = pl.ds(pl.multiple_of(ti * width, 128), width)

    def block(d):
        return pl.ds(d * cap, cap)

    def group(g):
        return pl.ds(g * group_rows, group_rows)

    def dispatch_copy(d):
        return remote(
            outg.at[block(d)], feats.at[block(d), own], d_s.at[d], d_r.at[d], {"ep": flip(me, d)}
        )

    def feat_x(g, j):
        ref = feats.at[group(g), own]
        where = {"tp": ((chip + j) % chips) * 2 + core}
        return remote(ref, ref, fx_s.at[g, j], fx_r.at[g, j], where)

    def feat_pair(g, j):
        source = ((chip + chips - j) % chips) * 2 + core
        ref = feats.at[group(g), pl.ds(pl.multiple_of(source * width, 128), width)]
        return remote(ref, ref, fp_s.at[g, j], fp_r.at[g, j], {"tp": partner})

    def share(g):
        for j in range(1, chips):
            go(feat_x(g, j))
        go(feat_pair(g, 0))

    def pass_on(g):
        for j in range(1, chips):
            feat_x(g, j).wait_recv()
            go(feat_pair(g, j))

    for d in range(n):
        base = float(d * cap)
        chosen = jnp.where(
            (target[0] == slot_iota + base) | (target[1] == slot_iota + base), 1.0, 0.0
        ).astype(bf16)
        picked = jnp.dot(chosen, normed, preferred_element_type=f32).astype(bf16)
        if d == 0:
            feats[block(0), own] = picked
        else:
            outg[block(d), :] = picked
            go(dispatch_copy(d))
        if d == per_group - 1 and per_group == 1:
            share(0)

    lane = lax.broadcasted_iota(jnp.int32, (rows, 128), 1).astype(f32)
    for k in range(2):
        column = to_column(target[k])
        for at in range(0, n * cap, 128):
            pick[k, :, at : at + 128] = jnp.where(column == lane + float(at), 1.0, 0.0).astype(bf16)

    chunk_groups = groups // len(order)

    def hid_ref(q, owner, i):
        at = pl.multiple_of(owner * units + i * n_tile, 128)
        return hid.at[pl.ds(q * chunk_groups * group_rows, chunk_groups * group_rows), pl.ds(at, n_tile)]

    def hid_x(q, i, j):
        ref = hid_ref(q, ti, i)
        where = {"tp": ((chip + j) % chips) * 2 + core}
        return remote(ref, ref, hx_s.at[q, i, j], hx_r.at[q, i, j], where)

    def hid_pair(q, i, j):
        ref = hid_ref(q, ((chip + chips - j) % chips) * 2 + core, i)
        return remote(ref, ref, hp_s.at[q, i, j], hp_r.at[q, i, j], {"tp": partner})

    def chunk(q):
        return pl.ds(q * chunk_groups * group_rows, chunk_groups * group_rows)

    def gate_up(q):
        for g in range(q * chunk_groups, (q + 1) * chunk_groups):
            for j in range(chips):
                feat_pair(g, j).wait_recv()

        def tile(i, carry):
            cols = pl.ds(pl.multiple_of(i * n_tile, 128), n_tile)
            x = feats[chunk(q), :]
            gate = jnp.dot(x, wg[:, cols], preferred_element_type=f32)
            upper = jnp.dot(x, wu[:, cols], preferred_element_type=f32)
            value = gate / (1.0 + jnp.exp(-gate)) * upper
            mine = pl.ds(pl.multiple_of(ti * units + i * n_tile, 128), n_tile)
            hid[chunk(q), mine] = value.astype(bf16)
            for j in range(1, chips):
                hid_x(q, i, j).start()
            hid_pair(q, i, 0).start()
            return carry

        lax.fori_loop(0, tiles, tile, 0)

    ready = {q: (q + 1) * chunk_groups - 1 for q in range(len(order))}
    state = {"done": 0, "weights": False}

    def advance(upto):
        while state["done"] < len(order) and max(
            ready[q] for q in order[: state["done"] + 1]
        ) <= upto:
            if not state["weights"]:
                loads[0].wait()
                loads[1].wait()
                state["weights"] = True
            gate_up(order[state["done"]])
            state["done"] += 1

    for g in range(groups):
        for d in range(g * per_group, (g + 1) * per_group):
            if d > 0:
                dispatch_copy(d).wait_recv()
        if not (g == 0 and per_group == 1):
            share(g)
        if g > 0:
            pass_on(g - 1)
            advance(g - 2)
    pass_on(groups - 1)
    advance(groups - 1)

    out_tile = min(256, width)

    def return_copy(d):
        return remote(back.at[block(d)], ret.at[block(d)], r_s.at[d], r_r.at[d], {"ep": flip(me, d)})

    loads[2].wait()
    for q in order:
        def relay(i, carry):
            for j in range(1, chips):
                hid_x(q, i, j).wait_recv()
                hid_pair(q, i, j).start()
            return carry

        def arrive(i, carry):
            for j in range(chips):
                hid_pair(q, i, j).wait_recv()
            return carry

        lax.fori_loop(0, tiles, relay, 0)
        lax.fori_loop(0, tiles, arrive, 0)

        def down(i, carry):
            cols = pl.ds(pl.multiple_of(i * out_tile, 128), out_tile)
            back[chunk(q), cols] = jnp.dot(
                hid[chunk(q), :], wd[:, cols], preferred_element_type=f32
            ).astype(bf16)
            return carry

        lax.fori_loop(0, width // out_tile, down, 0)
        first = q * chunk_groups * per_group
        for d in range(first, first + chunk_groups * per_group):
            if d > 0:
                go(return_copy(d))
    ret[block(0), :] = back[block(0), :]
    for d in range(1, n):
        return_copy(d).wait_recv()

    mixed = 0.0
    for k in range(2):
        picked = jnp.dot(pick[k], ret[...], preferred_element_type=f32)
        mixed = mixed + picked * to_column(rw_ref[k : k + 1, :])[:, 0:1]
    out_copies = total_over_tp(ss_out, so_s, so_r, row_sums(mixed * mixed))
    for copy in sent[: -len(out_copies)]:
        copy.wait_send()
    for q in order:
        def drain(i, carry):
            for j in range(1, chips):
                hid_x(q, i, j).wait_send()
            for j in range(chips):
                hid_pair(q, i, j).wait_send()
            return carry

        lax.fori_loop(0, tiles, drain, 0)
    for copy in out_copies:
        copy.wait_recv()
    total = ss_out[0]
    for j in range(1, tp):
        total = total + ss_out[j]
    scale = to_column(lax.rsqrt(total / (width * tp) + epsilon))[:, 0:1]
    out_ref[...] = (mixed * scale * post_ref[...]).astype(bf16)
    for copy in out_copies:
        copy.wait_send()


def on_device(
    tokens, expert_ids, route_weights, pre_gain, post_gain, gate_weight, up_weight, down_weight
):
    rows, width = tokens.shape
    n, tp = lax.axis_size("ep"), lax.axis_size("tp")
    assert gate_weight.shape[0] == 1 and expert_ids.shape[1] == 2
    capacity = max(2, rows * 2 * 5 // (4 * n))
    cap = -(-capacity // 16) * 16
    groups = min(8, n)
    order = (1, 2, 3, 0)
    slots = n * cap
    chips = tp // 2
    features, units = gate_weight.shape[1:]
    hidden_all = units * tp
    tiles = units // min(256, units)
    chunks = len(order)
    dma = pltpu.SemaphoreType.DMA
    vmem = pl.BlockSpec(memory_space=pltpu.VMEM)
    hbm = pl.BlockSpec(memory_space=pl.ANY)
    return pl.pallas_call(
        functools.partial(kernel, n, tp, capacity, cap, groups, order),
        out_shape=jax.ShapeDtypeStruct((rows, width), bf16),
        in_specs=[vmem] * 5 + [hbm] * 3,
        out_specs=vmem,
        scratch_shapes=[
            pltpu.VMEM((features, units), bf16),
            pltpu.VMEM((features, units), bf16),
            pltpu.VMEM((hidden_all, width), bf16),
            pltpu.VMEM((slots, width), bf16),
            pltpu.VMEM((slots, features), bf16),
            pltpu.VMEM((slots, hidden_all), bf16),
            pltpu.VMEM((slots, width), bf16),
            pltpu.VMEM((slots, width), bf16),
            pltpu.VMEM((2, rows, slots), bf16),
            pltpu.VMEM((tp, 1, rows), f32),
            pltpu.VMEM((tp, 1, rows), f32),
            dma((3,)),
            dma((tp,)), dma((tp,)), dma((tp,)), dma((tp,)),
            dma((n,)), dma((n,)),
            dma((groups, chips)), dma((groups, chips)),
            dma((groups, chips)), dma((groups, chips)),
            dma((chunks, tiles, chips)), dma((chunks, tiles, chips)),
            dma((chunks, tiles, chips)), dma((chunks, tiles, chips)),
            dma((n,)), dma((n,)),
        ],
        compiler_params=pltpu.CompilerParams(
            collective_id=0, has_side_effects=True, vmem_limit_bytes=56 * 1024 * 1024
        ),
    )(
        tokens, jnp.transpose(expert_ids), jnp.transpose(route_weights),
        pre_gain.reshape(1, -1), post_gain.reshape(1, -1),
        gate_weight, up_weight, down_weight,
    )


def solution(mesh):
    return jax.shard_map(
        on_device,
        mesh=mesh,
        in_specs=(
            P("ep", "tp"),
            P("ep", None),
            P("ep", None),
            P("tp"),
            P("tp"),
            P("ep", None, "tp"),
            P("ep", None, "tp"),
            P("ep", None, "tp"),
        ),
        out_specs=P("ep", "tp"),
        check_vma=False,
    )
```

```python
import functools

import jax
import jax.numpy as jnp
from jax import lax
from jax.experimental import pallas as pl
from jax.experimental.pallas import tpu as pltpu
from jax.sharding import PartitionSpec as P

epsilon = 1e-06
MESH = pl.DeviceIdType.MESH
f32, bf16 = jnp.float32, jnp.bfloat16


def flip(index, bits):
    out, bit = index, 1
    while bit <= bits:
        if bits & bit:
            out = out + bit * (1 - 2 * ((index // bit) % 2))
        bit *= 2
    return out


def to_column(row):
    return jnp.transpose(jnp.broadcast_to(row, (128, row.shape[1])))


def wide(column, width):
    return jnp.concatenate([column] * (width // 128), axis=1)


def row_sums(values):
    part = values[:, 0:128]
    for at in range(128, values.shape[1], 128):
        part = part + values[:, at : at + 128]
    return jnp.sum(jnp.transpose(part), axis=0, keepdims=True)


def kernel(
    n, tp, cap, groups, chunks, pieces,
    tok_ref, ids_ref, rw_ref, pre_ref, post_ref, wg_hbm, wu_hbm, wd_hbm,
    out_ref,
    wg, wu, wd, outg, feats, rows_in, hid, back, ret, gain, ss_out, mix, wcol, *rest,
):
    picks, sems = rest[: len(pieces)], rest[len(pieces) :]
    (w_sem, g_s, g_r, so_s, so_r, d_s, d_r, fx_s, fx_r, fp_s, fp_r,
     hx_s, hx_r, hp_s, hp_r, r_s, r_r) = sems
    me, ti = lax.axis_index("ep"), lax.axis_index("tp")
    chips = tp // 2
    chip, core = ti // 2, ti % 2
    partner = chip * 2 + (1 - core)
    rows, width = tok_ref.shape
    units = wg.shape[1]
    n_tile = min(256, units)
    tiles = units // n_tile
    per_group = n // groups
    group_rows = per_group * cap

    barrier = pltpu.get_barrier_semaphore()
    for d in range(1, n):
        pl.semaphore_signal(barrier, inc=1, device_id={"ep": flip(me, d)}, device_id_type=MESH)
    for j in range(1, tp):
        pl.semaphore_signal(barrier, inc=1, device_id={"tp": (ti + j) % tp}, device_id_type=MESH)
    loads = [
        pltpu.make_async_copy(src.at[0], dst, w_sem.at[i])
        for i, (src, dst) in enumerate(((wg_hbm, wg), (wu_hbm, wu), (wd_hbm, wd)))
    ]
    for load in loads:
        load.start()
    sent = []

    def remote(src, dst, s_sem, r_sem, where):
        return pltpu.make_async_remote_copy(
            src_ref=src, dst_ref=dst, send_sem=s_sem, recv_sem=r_sem,
            device_id=where, device_id_type=MESH,
        )

    def go(copy):
        copy.start()
        sent.append(copy)

    lanes = max(n, 16)
    rel = [jnp.bitwise_xor(ids_ref[k : k + 1, :], me) for k in range(2)]
    d_iota = lax.broadcasted_iota(jnp.int32, (lanes, rows), 0)
    hot = [jnp.where(rel[k] == d_iota, 1.0, 0.0).astype(f32) for k in range(2)]
    earlier = jnp.where(
        lax.broadcasted_iota(jnp.int32, (rows, rows), 0)
        < lax.broadcasted_iota(jnp.int32, (rows, rows), 1), 1.0, 0.0,
    ).astype(bf16)
    prefix = jnp.dot((hot[0] + hot[1]).astype(bf16), earlier, preferred_element_type=f32)
    target = [
        rel[k].astype(f32) * cap + jnp.sum(prefix * hot[k], axis=0, keepdims=True)
        for k in range(2)
    ]
    slot_iota = lax.broadcasted_iota(jnp.int32, (cap, rows), 0).astype(f32)

    tokens = tok_ref[...]
    own = pl.ds(pl.multiple_of(ti * width, 128), width)

    def block(d):
        return pl.ds(d * cap, cap)

    def group(g):
        return pl.ds(g * group_rows, group_rows)

    def dispatch_copy(d):
        return remote(
            outg.at[block(d)], feats.at[block(d), own], d_s.at[d], d_r.at[d], {"ep": flip(me, d)}
        )

    def feat_x(g, j):
        ref = feats.at[group(g), own]
        where = {"tp": ((chip + j) % chips) * 2 + core}
        return remote(ref, ref, fx_s.at[g, j], fx_r.at[g, j], where)

    def feat_pair(g, j):
        source = ((chip + chips - j) % chips) * 2 + core
        ref = feats.at[group(g), pl.ds(pl.multiple_of(source * width, 128), width)]
        return remote(ref, ref, fp_s.at[g, j], fp_r.at[g, j], {"tp": partner})

    def share(g):
        for j in range(1, chips):
            go(feat_x(g, j))
        go(feat_pair(g, 0))

    def pass_on(g):
        for j in range(1, chips):
            feat_x(g, j).wait_recv()
            go(feat_pair(g, j))

    for d in range(n):
        base = float(d * cap)
        chosen = jnp.where(
            (target[0] == slot_iota + base) | (target[1] == slot_iota + base), 1.0, 0.0
        ).astype(bf16)
        picked = jnp.dot(chosen, tokens, preferred_element_type=f32).astype(bf16)
        if d == 0:
            feats[block(0), own] = picked
        else:
            outg[block(d), :] = picked
    pl.semaphore_wait(barrier, n - 1 + tp - 1)
    if per_group == 1:
        share(0)
    for d in range(1, n):
        go(dispatch_copy(d))
    gain[:, own] = pre_ref[...]

    def gain_copy(j):
        return remote(pre_ref, gain.at[:, own], g_s.at[j], g_r.at[j], {"tp": (ti + j) % tp})

    for j in range(1, tp):
        go(gain_copy(j))

    def piece_slots(piece):
        return pl.ds(piece[0] * group_rows, piece[1] * group_rows)

    for k in range(2):
        column = to_column(target[k])
        wcol[k] = to_column(rw_ref[k : k + 1, :])
        for piece, pick in zip(pieces, picks):
            base = piece[0] * group_rows
            for at in range(0, pick.shape[2], 128):
                size = min(128, pick.shape[2] - at)
                lane = lax.broadcasted_iota(jnp.int32, (rows, size), 1).astype(f32)
                pick[k, :, at : at + size] = jnp.where(
                    column[:, 0:size] == lane + float(base + at), 1.0, 0.0
                ).astype(bf16)

    def combine(piece, pick, first):
        value = 0.0 if first else mix[...]
        for k in range(2):
            found = jnp.dot(pick[k], ret[piece_slots(piece), :], preferred_element_type=f32)
            value = value + found * wide(wcol[k], width)
        return value

    def chunk(q):
        return pl.ds(chunks[q][0] * group_rows, chunks[q][1] * group_rows)

    def hid_ref(q, owner, i):
        at = pl.multiple_of(owner * units + i * n_tile, 128)
        return hid.at[chunk(q), pl.ds(at, n_tile)]

    def hid_x(q, i, j):
        ref = hid_ref(q, ti, i)
        where = {"tp": ((chip + j) % chips) * 2 + core}
        return remote(ref, ref, hx_s.at[q, i, j], hx_r.at[q, i, j], where)

    def hid_pair(q, i, j):
        ref = hid_ref(q, ((chip + chips - j) % chips) * 2 + core, i)
        return remote(ref, ref, hp_s.at[q, i, j], hp_r.at[q, i, j], {"tp": partner})

    def send_tile(q, i):
        for j in range(1, chips):
            hid_x(q, i, j).start()
        hid_pair(q, i, 0).start()

    def send_hidden(q):
        def body(i, carry):
            send_tile(q, i)
            return carry

        lax.fori_loop(0, tiles, body, 0)

    def gate_up(first, many, q=None):
        for g in range(first, first + many):
            for j in range(chips):
                feat_pair(g, j).wait_recv()

        at, count = first * group_rows, many * group_rows
        span = pl.ds(at, count)
        batch = max(u for u in range(1, 6) if (count // 16) % u == 0)

        def norm(i, carry):
            for u in range(batch):
                here = (i * batch + u) * 16
                part = pl.ds(pl.multiple_of(at + here, 16), 16)
                x = feats[part, :].astype(f32)
                square = jnp.sum(x * x, axis=1, keepdims=True)
                x = x * lax.rsqrt(square / (width * tp) + epsilon) * gain[...]
                rows_in[pl.ds(pl.multiple_of(here, 16), 16), :] = x.astype(bf16)
            return carry

        lax.fori_loop(0, count // (16 * batch), norm, 0)

        def tile(i, carry):
            cols = pl.ds(pl.multiple_of(i * n_tile, 128), n_tile)
            x = rows_in[0:count, :]
            gate = jnp.dot(x, wg[:, cols], preferred_element_type=f32)
            upper = jnp.dot(x, wu[:, cols], preferred_element_type=f32)
            value = gate / (1.0 + jnp.exp(-gate)) * upper
            mine = pl.ds(pl.multiple_of(ti * units + i * n_tile, 128), n_tile)
            hid[span, mine] = value.astype(bf16)
            if q is not None:
                send_tile(q, i)
            return carry

        lax.fori_loop(0, tiles, tile, 0)

    def take(g):
        for d in range(g * per_group, (g + 1) * per_group):
            if d > 0:
                dispatch_copy(d).wait_recv()
        if not (g == 0 and per_group == 1):
            share(g)

    out_tile = min(256, width)

    def return_copy(d):
        return remote(back.at[block(d)], ret.at[block(d)], r_s.at[d], r_r.at[d], {"ep": flip(me, d)})

    def finish(q):
        def relay(i, carry):
            for j in range(1, chips):
                hid_x(q, i, j).wait_recv()
                hid_pair(q, i, j).start()
            return carry

        def arrive(i, carry):
            for j in range(chips):
                hid_pair(q, i, j).wait_recv()
            return carry

        lax.fori_loop(0, tiles, relay, 0)
        lax.fori_loop(0, tiles, arrive, 0)

        def down(i, carry):
            cols = pl.ds(pl.multiple_of(i * out_tile, 128), out_tile)
            back[chunk(q), cols] = jnp.dot(
                hid[chunk(q), :], wd[:, cols], preferred_element_type=f32
            ).astype(bf16)
            return carry

        lax.fori_loop(0, width // out_tile, down, 0)
        for d in range(chunks[q][0] * per_group, sum(chunks[q]) * per_group):
            if d > 0:
                go(return_copy(d))
        if chunks[q][0] == 0:
            ret[block(0), :] = back[block(0), :]

    take(0)
    for g in range(1, 6):
        take(g)
        if g > 1:
            pass_on(g - 2)
    loads[0].wait()
    loads[1].wait()
    for j in range(1, tp):
        gain_copy(j).wait_recv()
    gate_up(2, 2, 0)
    pass_on(4)
    take(6)
    take(7)
    pass_on(5)
    gate_up(4, 2, 1)
    gate_up(0, 2)
    loads[2].wait()
    finish(0)
    pass_on(6)
    pass_on(7)
    gate_up(6, 2, 2)
    send_hidden(3)
    send_hidden(4)
    finish(1)
    finish(2)
    finish(3)
    piece = pieces[0]
    for d in range(piece[0] * per_group, sum(piece) * per_group):
        return_copy(d).wait_recv()
    mix[...] = combine(piece, picks[0], True)
    finish(4)
    for piece, pick in zip(pieces[1:], picks[1:]):
        for d in range(piece[0] * per_group, sum(piece) * per_group):
            if d > 0:
                return_copy(d).wait_recv()
        mix[...] = combine(piece, pick, False)
    mixed = mix[...]
    ss_out[0] = row_sums(mixed * mixed)
    out_copies = [
        remote(ss_out.at[0], ss_out.at[j], so_s.at[j], so_r.at[j], {"tp": (ti + j) % tp})
        for j in range(1, tp)
    ]
    for copy in out_copies:
        copy.start()
    for copy in sent:
        copy.wait_send()
    for q in range(len(chunks)):
        def drain(i, carry):
            for j in range(1, chips):
                hid_x(q, i, j).wait_send()
            for j in range(chips):
                hid_pair(q, i, j).wait_send()
            return carry

        lax.fori_loop(0, tiles, drain, 0)
    for copy in out_copies:
        copy.wait_recv()
    total = ss_out[0]
    for j in range(1, tp):
        total = total + ss_out[j]
    scale = wide(to_column(lax.rsqrt(total / (width * tp) + epsilon)), width)
    out_ref[...] = (mixed * scale * post_ref[...]).astype(bf16)
    for copy in out_copies:
        copy.wait_send()


def on_device(
    tokens, expert_ids, route_weights, pre_gain, post_gain, gate_weight, up_weight, down_weight
):
    rows, width = tokens.shape
    n, tp = lax.axis_size("ep"), lax.axis_size("tp")
    assert gate_weight.shape[0] == 1 and expert_ids.shape[1] == 2
    capacity = max(2, rows * 2 * 5 // (4 * n))
    cap = -(-capacity // 16) * 16
    groups = 8
    assert n % groups == 0
    chunks = ((2, 2), (4, 2), (6, 2), (1, 1), (0, 1))
    pieces = ((2, 4), (6, 2), (0, 2))
    slots = n * cap
    chips = tp // 2
    features, units = gate_weight.shape[1:]
    hidden_all = units * tp
    tiles = units // min(256, units)
    steps = len(chunks)
    most = max(count for _, count in chunks) * (slots // groups)
    dma = pltpu.SemaphoreType.DMA
    vmem = pl.BlockSpec(memory_space=pltpu.VMEM)
    hbm = pl.BlockSpec(memory_space=pl.ANY)
    return pl.pallas_call(
        functools.partial(kernel, n, tp, cap, groups, chunks, pieces),
        out_shape=jax.ShapeDtypeStruct((rows, width), bf16),
        in_specs=[vmem] * 5 + [hbm] * 3,
        out_specs=vmem,
        scratch_shapes=[
            pltpu.VMEM((features, units), bf16),
            pltpu.VMEM((features, units), bf16),
            pltpu.VMEM((hidden_all, width), bf16),
            pltpu.VMEM((slots, width), bf16),
            pltpu.VMEM((slots, features), bf16),
            pltpu.VMEM((most, features), bf16),
            pltpu.VMEM((slots, hidden_all), bf16),
            pltpu.VMEM((slots, width), bf16),
            pltpu.VMEM((slots, width), bf16),
            pltpu.VMEM((1, features), f32),
            pltpu.VMEM((tp, 1, rows), f32),
            pltpu.VMEM((rows, width), f32),
            pltpu.VMEM((2, rows, 128), f32),
            *[pltpu.VMEM((2, rows, count * (slots // groups)), bf16) for _, count in pieces],
            dma((3,)),
            dma((tp,)), dma((tp,)), dma((tp,)), dma((tp,)),
            dma((n,)), dma((n,)),
            dma((groups, chips)), dma((groups, chips)),
            dma((groups, chips)), dma((groups, chips)),
            dma((steps, tiles, chips)), dma((steps, tiles, chips)),
            dma((steps, tiles, chips)), dma((steps, tiles, chips)),
            dma((n,)), dma((n,)),
        ],
        compiler_params=pltpu.CompilerParams(
            collective_id=0, has_side_effects=True, vmem_limit_bytes=56 * 1024 * 1024
        ),
    )(
        tokens, jnp.transpose(expert_ids), jnp.transpose(route_weights),
        pre_gain.reshape(1, -1), post_gain.reshape(1, -1),
        gate_weight, up_weight, down_weight,
    )


def solution(mesh):
    return jax.shard_map(
        on_device,
        mesh=mesh,
        in_specs=(
            P("ep", "tp"),
            P("ep", None),
            P("ep", None),
            P("tp"),
            P("tp"),
            P("ep", None, "tp"),
            P("ep", None, "tp"),
            P("ep", None, "tp"),
        ),
        out_specs=P("ep", "tp"),
        check_vma=False,
    )
```

```python
import functools

import jax
import jax.numpy as jnp
from jax import lax
from jax.experimental import pallas as pl
from jax.experimental.pallas import tpu as pltpu
from jax.sharding import PartitionSpec as P

epsilon = 1e-06
MESH = pl.DeviceIdType.MESH
f32, bf16 = jnp.float32, jnp.bfloat16


def flip(index, bits):
    out, bit = index, 1
    while bit <= bits:
        if bits & bit:
            out = out + bit * (1 - 2 * ((index // bit) % 2))
        bit *= 2
    return out


def to_column(row):
    return jnp.transpose(jnp.broadcast_to(row, (128, row.shape[1])))


def wide(column, width):
    return jnp.concatenate([column] * (width // 128), axis=1)


def row_sums(values):
    part = values[:, 0:128]
    for at in range(128, values.shape[1], 128):
        part = part + values[:, at : at + 128]
    return jnp.sum(jnp.transpose(part), axis=0, keepdims=True)


def kernel(
    n, tp, cap, groups, chunks, pieces,
    tok_ref, ids_ref, rw_ref, pre_ref, post_ref, wg_hbm, wu_hbm, wd_hbm,
    out_ref,
    wg, wu, wd, outg, feats, rows_in, hid, back, ret, gain, ss_out, mix, wcol, *rest,
):
    picks, sems = rest[: len(pieces)], rest[len(pieces) :]
    (w_sem, g_s, g_r, so_s, so_r, d_s, d_r, fx_s, fx_r, fp_s, fp_r,
     hx_s, hx_r, hp_s, hp_r, r_s, r_r) = sems
    me, ti = lax.axis_index("ep"), lax.axis_index("tp")
    chips = tp // 2
    chip, core = ti // 2, ti % 2
    partner = chip * 2 + (1 - core)
    rows, width = tok_ref.shape
    units = wg.shape[1]
    n_tile = min(256, units)
    tiles = units // n_tile
    per_group = n // groups
    group_rows = per_group * cap

    barrier = pltpu.get_barrier_semaphore()
    for d in range(1, n):
        pl.semaphore_signal(barrier, inc=1, device_id={"ep": flip(me, d)}, device_id_type=MESH)
    for j in range(1, tp):
        pl.semaphore_signal(barrier, inc=1, device_id={"tp": (ti + j) % tp}, device_id_type=MESH)
    loads = [
        pltpu.make_async_copy(src.at[0], dst, w_sem.at[i])
        for i, (src, dst) in enumerate(((wg_hbm, wg), (wu_hbm, wu), (wd_hbm, wd)))
    ]
    for load in loads:
        load.start()

    def remote(src, dst, s_sem, r_sem, where):
        return pltpu.make_async_remote_copy(
            src_ref=src, dst_ref=dst, send_sem=s_sem, recv_sem=r_sem,
            device_id=where, device_id_type=MESH,
        )

    def go(copy):
        copy.start()

    lanes = max(n, 16)
    rel = [jnp.bitwise_xor(ids_ref[k : k + 1, :], me) for k in range(2)]
    d_iota = lax.broadcasted_iota(jnp.int32, (lanes, rows), 0)
    hot = [jnp.where(rel[k] == d_iota, 1.0, 0.0).astype(f32) for k in range(2)]
    earlier = jnp.where(
        lax.broadcasted_iota(jnp.int32, (rows, rows), 0)
        < lax.broadcasted_iota(jnp.int32, (rows, rows), 1), 1.0, 0.0,
    ).astype(bf16)
    prefix = jnp.dot((hot[0] + hot[1]).astype(bf16), earlier, preferred_element_type=f32)
    target = [
        rel[k].astype(f32) * cap + jnp.sum(prefix * hot[k], axis=0, keepdims=True)
        for k in range(2)
    ]
    slot_iota = lax.broadcasted_iota(jnp.int32, (cap, rows), 0).astype(f32)

    tokens = tok_ref[...]
    own = pl.ds(pl.multiple_of(ti * width, 128), width)

    def block(d):
        return pl.ds(d * cap, cap)

    def group(g):
        return pl.ds(g * group_rows, group_rows)

    def dispatch_copy(d):
        return remote(
            outg.at[block(d)], feats.at[block(d), own], d_s.at[0], d_r.at[d - 1], {"ep": flip(me, d)}
        )

    def feat_x(g, j):
        ref = feats.at[group(g), own]
        where = {"tp": ((chip + j) % chips) * 2 + core}
        return remote(ref, ref, fx_s.at[0], fx_r.at[g, j - 1], where)

    def feat_pair(g, j):
        source = ((chip + chips - j) % chips) * 2 + core
        ref = feats.at[group(g), pl.ds(pl.multiple_of(source * width, 128), width)]
        return remote(ref, ref, fp_s.at[0], fp_r.at[g], {"tp": partner})

    def share(g):
        for j in range(1, chips):
            go(feat_x(g, j))
        go(feat_pair(g, 0))

    def pass_on(g):
        for j in range(1, chips):
            feat_x(g, j).wait_recv()
            go(feat_pair(g, j))

    for d in range(n):
        base = float(d * cap)
        chosen = jnp.where(
            (target[0] == slot_iota + base) | (target[1] == slot_iota + base), 1.0, 0.0
        ).astype(bf16)
        picked = jnp.dot(chosen, tokens, preferred_element_type=f32).astype(bf16)
        if d == 0:
            feats[block(0), own] = picked
        else:
            outg[block(d), :] = picked
    pl.semaphore_wait(barrier, n - 1 + tp - 1)
    if per_group == 1:
        share(0)
    for d in range(1, n):
        go(dispatch_copy(d))
    gain[:, own] = pre_ref[...]

    def gain_copy(j):
        return remote(pre_ref, gain.at[:, own], g_s.at[0], g_r.at[j - 1], {"tp": (ti + j) % tp})

    for j in range(1, tp):
        go(gain_copy(j))

    def piece_slots(piece):
        return pl.ds(piece[0] * group_rows, piece[1] * group_rows)

    for k in range(2):
        column = to_column(target[k])
        wcol[k] = to_column(rw_ref[k : k + 1, :])
        for piece, pick in zip(pieces, picks):
            base = piece[0] * group_rows
            for at in range(0, pick.shape[2], 128):
                size = min(128, pick.shape[2] - at)
                lane = lax.broadcasted_iota(jnp.int32, (rows, size), 1).astype(f32)
                pick[k, :, at : at + size] = jnp.where(
                    column[:, 0:size] == lane + float(base + at), 1.0, 0.0
                ).astype(bf16)

    def combine(piece, pick, first):
        value = 0.0 if first else mix[...]
        for k in range(2):
            found = jnp.dot(pick[k], ret[piece_slots(piece), :], preferred_element_type=f32)
            value = value + found * wide(wcol[k], width)
        return value

    def chunk(q):
        return pl.ds(chunks[q][0] * group_rows, chunks[q][1] * group_rows)

    def hid_ref(q, owner, i):
        at = pl.multiple_of(owner * units + i * n_tile, 128)
        return hid.at[chunk(q), pl.ds(at, n_tile)]

    def hid_x(q, i, j):
        ref = hid_ref(q, ti, i)
        where = {"tp": ((chip + j) % chips) * 2 + core}
        return remote(ref, ref, hx_s.at[0], hx_r.at[q, i, j - 1], where)

    def hid_pair(q, i, j):
        ref = hid_ref(q, ((chip + chips - j) % chips) * 2 + core, i)
        return remote(ref, ref, hp_s.at[0], hp_r.at[q], {"tp": partner})

    def send_tile(q, i):
        for j in range(1, chips):
            hid_x(q, i, j).start()
        hid_pair(q, i, 0).start()

    def send_hidden(q):
        def body(i, carry):
            send_tile(q, i)
            return carry

        lax.fori_loop(0, tiles, body, 0)

    def gate_up(first, many, q=None):
        for g in range(first, first + many):
            ref = feats.at[group(g), 0 : chips * width]
            remote(ref, ref, fp_s.at[0], fp_r.at[g], {"tp": partner}).wait_recv()

        at, count = first * group_rows, many * group_rows
        span = pl.ds(at, count)
        batch = max(u for u in range(1, 6) if (count // 16) % u == 0)

        def norm(i, carry):
            for u in range(batch):
                here = (i * batch + u) * 16
                part = pl.ds(pl.multiple_of(at + here, 16), 16)
                x = feats[part, :].astype(f32)
                square = jnp.sum(x * x, axis=1, keepdims=True)
                x = x * lax.rsqrt(square / (width * tp) + epsilon) * gain[...]
                rows_in[pl.ds(pl.multiple_of(here, 16), 16), :] = x.astype(bf16)
            return carry

        lax.fori_loop(0, count // (16 * batch), norm, 0)

        def tile(i, carry):
            cols = pl.ds(pl.multiple_of(i * n_tile, 128), n_tile)
            x = rows_in[0:count, :]
            gate = jnp.dot(x, wg[:, cols], preferred_element_type=f32)
            upper = jnp.dot(x, wu[:, cols], preferred_element_type=f32)
            value = gate / (1.0 + jnp.exp(-gate)) * upper
            mine = pl.ds(pl.multiple_of(ti * units + i * n_tile, 128), n_tile)
            hid[span, mine] = value.astype(bf16)
            if q is not None:
                send_tile(q, i)
            return carry

        lax.fori_loop(0, tiles, tile, 0)

    def take(g):
        for d in range(g * per_group, (g + 1) * per_group):
            if d > 0:
                dispatch_copy(d).wait_recv()
        if not (g == 0 and per_group == 1):
            share(g)

    out_tile = min(256, width)

    def return_copy(d):
        return remote(back.at[block(d)], ret.at[block(d)], r_s.at[0], r_r.at[d - 1], {"ep": flip(me, d)})

    def finish(q):
        def relay(i, carry):
            for j in range(1, chips):
                hid_x(q, i, j).wait_recv()
                hid_pair(q, i, j).start()
            return carry

        lax.fori_loop(0, tiles, relay, 0)
        ref = hid.at[chunk(q), 0 : chips * units]
        remote(ref, ref, hp_s.at[0], hp_r.at[q], {"tp": partner}).wait_recv()

        def down(i, carry):
            cols = pl.ds(pl.multiple_of(i * out_tile, 128), out_tile)
            back[chunk(q), cols] = jnp.dot(
                hid[chunk(q), :], wd[:, cols], preferred_element_type=f32
            ).astype(bf16)
            return carry

        lax.fori_loop(0, width // out_tile, down, 0)
        for d in range(chunks[q][0] * per_group, sum(chunks[q]) * per_group):
            if d > 0:
                go(return_copy(d))
        if chunks[q][0] == 0:
            ret[block(0), :] = back[block(0), :]

    take(0)
    for g in range(1, 6):
        take(g)
        if g > 1:
            pass_on(g - 2)
    loads[0].wait()
    loads[1].wait()
    for j in range(1, tp):
        gain_copy(j).wait_recv()
    gate_up(2, 2, 0)
    pass_on(4)
    take(6)
    take(7)
    pass_on(5)
    gate_up(4, 2, 1)
    gate_up(0, 2)
    loads[2].wait()
    finish(0)
    pass_on(6)
    pass_on(7)
    gate_up(6, 2, 2)
    send_hidden(3)
    send_hidden(4)
    finish(1)
    finish(2)
    finish(3)
    piece = pieces[0]
    for d in range(piece[0] * per_group, sum(piece) * per_group):
        return_copy(d).wait_recv()
    mix[...] = combine(piece, picks[0], True)
    finish(4)
    for piece, pick in zip(pieces[1:], picks[1:]):
        for d in range(piece[0] * per_group, sum(piece) * per_group):
            if d > 0:
                return_copy(d).wait_recv()
        mix[...] = combine(piece, pick, False)
    mixed = mix[...]
    ss_out[0] = row_sums(mixed * mixed)
    out_copies = [
        remote(ss_out.at[0], ss_out.at[j], so_s.at[0], so_r.at[j - 1], {"tp": (ti + j) % tp})
        for j in range(1, tp)
    ]
    for copy in out_copies:
        copy.start()
    def drain(ref, sem):
        remote(ref, ref, sem.at[0], so_r.at[0], {"tp": partner}).wait_send()

    later = pl.ds(cap, (n - 1) * cap)
    drain(outg.at[later], d_s)
    drain(back.at[later], r_s)
    drain(gain.at[:, 0 : (tp - 1) * width], g_s)
    drain(feats.at[:, 0 : (chips - 1) * width], fx_s)
    drain(feats.at[:, 0 : chips * width], fp_s)
    drain(hid.at[:, 0 : (chips - 1) * units], hx_s)
    drain(hid.at[:, 0 : chips * units], hp_s)
    for copy in out_copies:
        copy.wait_recv()
    total = ss_out[0]
    for j in range(1, tp):
        total = total + ss_out[j]
    scale = wide(to_column(lax.rsqrt(total / (width * tp) + epsilon)), width)
    out_ref[...] = (mixed * scale * post_ref[...]).astype(bf16)
    drain(ss_out.at[0 : tp - 1], so_s)


def on_device(
    tokens, expert_ids, route_weights, pre_gain, post_gain, gate_weight, up_weight, down_weight
):
    rows, width = tokens.shape
    n, tp = lax.axis_size("ep"), lax.axis_size("tp")
    assert gate_weight.shape[0] == 1 and expert_ids.shape[1] == 2
    capacity = max(2, rows * 2 * 5 // (4 * n))
    cap = -(-capacity // 16) * 16
    groups = 8
    assert n % groups == 0
    chunks = ((2, 2), (4, 2), (6, 2), (1, 1), (0, 1))
    pieces = ((2, 4), (6, 2), (0, 2))
    slots = n * cap
    chips = tp // 2
    features, units = gate_weight.shape[1:]
    hidden_all = units * tp
    tiles = units // min(256, units)
    steps = len(chunks)
    most = max(count for _, count in chunks) * (slots // groups)
    dma = pltpu.SemaphoreType.DMA
    vmem = pl.BlockSpec(memory_space=pltpu.VMEM)
    hbm = pl.BlockSpec(memory_space=pl.ANY)
    return pl.pallas_call(
        functools.partial(kernel, n, tp, cap, groups, chunks, pieces),
        out_shape=jax.ShapeDtypeStruct((rows, width), bf16),
        in_specs=[vmem] * 5 + [hbm] * 3,
        out_specs=vmem,
        scratch_shapes=[
            pltpu.VMEM((features, units), bf16),
            pltpu.VMEM((features, units), bf16),
            pltpu.VMEM((hidden_all, width), bf16),
            pltpu.VMEM((slots, width), bf16),
            pltpu.VMEM((slots, features), bf16),
            pltpu.VMEM((most, features), bf16),
            pltpu.VMEM((slots, hidden_all), bf16),
            pltpu.VMEM((slots, width), bf16),
            pltpu.VMEM((slots, width), bf16),
            pltpu.VMEM((1, features), f32),
            pltpu.VMEM((tp, 1, rows), f32),
            pltpu.VMEM((rows, width), f32),
            pltpu.VMEM((2, rows, 128), f32),
            *[pltpu.VMEM((2, rows, count * (slots // groups)), bf16) for _, count in pieces],
            dma((3,)),
            dma((1,)), dma((tp - 1,)), dma((1,)), dma((tp - 1,)),
            dma((1,)), dma((n - 1,)),
            dma((1,)), dma((groups, chips - 1)),
            dma((1,)), dma((groups,)),
            dma((1,)), dma((steps, tiles, chips - 1)),
            dma((1,)), dma((steps,)),
            dma((1,)), dma((n - 1,)),
        ],
        compiler_params=pltpu.CompilerParams(
            collective_id=0, has_side_effects=True, vmem_limit_bytes=56 * 1024 * 1024
        ),
    )(
        tokens, jnp.transpose(expert_ids), jnp.transpose(route_weights),
        pre_gain.reshape(1, -1), post_gain.reshape(1, -1),
        gate_weight, up_weight, down_weight,
    )


def solution(mesh):
    return jax.shard_map(
        on_device,
        mesh=mesh,
        in_specs=(
            P("ep", "tp"),
            P("ep", None),
            P("ep", None),
            P("tp"),
            P("tp"),
            P("ep", None, "tp"),
            P("ep", None, "tp"),
            P("ep", None, "tp"),
        ),
        out_specs=P("ep", "tp"),
        check_vma=False,
    )
```
